32 devices in a mesh: grp: 2 (over y), ep: 8 (over z, core), tp: 2 (over x).
Axes of the slice: x: 2, y: 2, z: 4, core: 2. Of those that a mesh axis runs over, the one named last changes fastest.
Arguments:
- resid_in: bfloat16 [176, 2048], P(('grp', 'ep')), parts along dimension 0, may hold values from -6 to 6
- norm_attn: float32 [2048], replicated, may hold values from 0.1 to 1.9
- norm_moe: float32 [2048], replicated, may hold values from 0.1 to 1.9
- w_query: bfloat16 [2048, 1024], P('ep', 'tp'), may hold values from -0.125 to 0.125
- w_key: bfloat16 [2048, 256], P('ep', 'tp'), may hold values from -0.125 to 0.125
- w_value: bfloat16 [2048, 256], P('ep', 'tp'), may hold values from -0.125 to 0.125
- head_offset: float32 [16], P('tp'), may hold values from 1.5 to 9.5
- kv_cache: bfloat16 [176, 1024, 4, 128], P(('grp', 'ep'), None, 'tp'), parts along dimension 0, may hold values from -6 to 6
- lengths: int32 [176], P(('grp', 'ep')), parts along dimension 0, may hold values from 128 to 1024, as said below
- w_output: bfloat16 [1024, 2048], P('tp', 'ep'), may hold values from -0.375 to 0.375
- routes: int32 [176, 4], P(('grp', 'ep')), parts along dimension 0, may hold values from 0 to 7, all different within a row; in each aligned block of 11 rows (0 to 10, 11 to 21, ...) at most 7 rows name the same one
- route_weights: float32 [176, 4], P(('grp', 'ep')), parts along dimension 0, may hold values from 0.2 to 1
- gate_experts: bfloat16 [8, 2048, 512], P('ep', None, 'tp'), may hold values from -0.125 to 0.125
- up_experts: bfloat16 [8, 2048, 512], P('ep', None, 'tp'), may hold values from -0.125 to 0.125
- down_experts: bfloat16 [8, 512, 2048], P('ep', 'tp'), may hold values from -0.25 to 0.25
- gate_shared: bfloat16 [2048, 512], P('ep', 'tp'), may hold values from -0.125 to 0.125
- up_shared: bfloat16 [2048, 512], P('ep', 'tp'), may hold values from -0.125 to 0.125
- down_shared: bfloat16 [512, 2048], P('tp', 'ep'), may hold values from -0.25 to 0.25
Outputs:
- layer_out: bfloat16 [176, 2048], P(('grp', 'ep'), 'tp'), parts along dimension 0
- new_rows: bfloat16 [176, 4, 128], P(('grp', 'ep'), 'tp'), parts along dimension 0
The draws below stay inside these ranges and needn't reach their ends.
There are 2 independent parts, one for each index of `grp`. The reference program is written for one: setup_inputs(seed, part) draws one part's arguments, and reference() takes and returns one part's arrays. A program takes and returns all parts, laid end to end along the dimension named above; an argument that names none is the same for every part. Nothing has to cross between parts.
Inputs may be any that keep to these rules, and one draw needn't show every extreme that they name: `routes`: among the rows of one device no expert is named more than 7 times, and in every draw some expert is named exactly 7 times by one device's rows; a row names 4 different experts. Sequence b's new token follows cache positions 0 to lengths[b] - 1; the other positions are not read.
All inputs are finite; a program needn't handle non-finite values.
Results may differ from the reference program's by a relative error of at most 0.015.
Values may be sent and summed in bfloat16 or wider, within the bound.
No kernel may reach another device: no remote copies, remote signals or barrier semaphores. Data moves between devices by JAX's collectives and lax.ppermute only.
A program may use at most 64 MiB of HBM per device.

```python
import math
import jax
import jax.numpy as jnp
import numpy as np
from jax import lax

D = 2048
HEADS = 16
KV_HEADS = 4
HEAD = 64
FE = 512
FS = 512
TOPK = 4
LEN = 1024
SEQ_DEV = 11
EXPERTS = 8
TOKENS = 88
CAP = 7
N_EP = 8
N_TP = 2


def draw_head_offset(key, part):
    key_one, key_two = jax.random.split(key)
    order = jax.random.permutation(key_two, HEADS)
    fast_rate = jax.random.uniform(key_one, (HEADS,), jnp.float32, 1.5, 3.0)
    slow_rate = jax.random.uniform(jax.random.fold_in(key_one, 7), (HEADS,), jnp.float32, 6.5, 9.0)
    return jnp.where(order < HEADS // 2, fast_rate, slow_rate)


def draw_lengths(key, part):
    key_one, key_two = jax.random.split(key)
    drawn = jax.random.randint(key_one, (TOKENS,), LEN // 8, LEN + 1, dtype=jnp.int32)
    chosen = jax.random.randint(key_two, (), 0, TOKENS, dtype=jnp.int32)
    drawn = drawn.at[chosen].set(LEN)
    return drawn.at[(chosen + 1) % TOKENS].set(LEN // 8)


def level_of(stream_key, shape, cuts, least, high):
    def one(axis_at, blocks):
        steps = jax.random.uniform(jax.random.fold_in(jax.random.fold_in(stream_key, 6), axis_at), (blocks,), jnp.float32, least / len(cuts), high / len(cuts))
        return jnp.repeat(jnp.exp(steps), shape[axis_at] // blocks).reshape((-1,) + (1,) * (len(shape) - axis_at - 1))

    factor_of = one(*cuts[0])
    for cut in cuts[1:]:
        factor_of = factor_of * one(*cut)
    return factor_of


def routed_block(rng, own, number, rows, amount, top, most, lean):
    order = jax.random.permutation(rng, amount)
    crowded, ordinary = portions_of(amount, rows * top, most, lean, True), portions_of(amount, rows * top, most, lean, False)
    places = jnp.arange(amount)

    def named(sizes, turn):
        used = int((sizes > 0).sum())
        fixed = max(1, used // 4)
        moved = fixed + (places - fixed + turn * (used - fixed)) % max(1, amount - fixed)
        return jnp.zeros((amount,), jnp.int32).at[order[jnp.where(places < fixed, places, moved)]].set(jnp.asarray(sizes, jnp.int32))

    sizes = jnp.where(number % 4 == 0, named(crowded, number // 4), named(ordinary, number - number // 4 - 1))
    mixed = jax.random.permutation(jax.random.fold_in(own, 3), amount)
    giver, sink = mixed[0:amount // 2 * 2:2], mixed[1:amount // 2 * 2:2]
    margin = jnp.minimum(sizes[giver] - 1, most - sizes[sink]) // 2
    margin = jnp.where((giver == order[0]) | (sink == order[0]) | (sizes[sink] == 0), 0, jnp.maximum(margin, 0))
    moved = jax.random.randint(jax.random.fold_in(own, 4), (amount // 2,), 0, 1 << 20) % (margin + 1)
    sizes = sizes.at[giver].add(-moved).at[sink].add(moved)
    labels = jnp.searchsorted(jnp.cumsum(sizes), jnp.arange(rows * top), side="right").astype(jnp.int32)
    grid = labels.reshape(top, rows).T
    grid = grid[jax.random.permutation(jax.random.fold_in(own, 1), rows)]
    turn = jax.random.randint(jax.random.fold_in(own, 2), (rows, 1), 0, top)
    return jnp.take_along_axis(grid, (jnp.arange(top)[None, :] + turn) % top, axis=1)


def portions_of(count, total, most, skew, full):
    loads = [(1 << 20) // math.isqrt(grade ** skew) + 1 for grade in range(1, count + 1)]
    largest = most if full else min(most, max(-(-total // count), total * loads[0] // sum(loads)))
    least = 1 if total - largest >= count - 1 else 0
    given, rest = [largest] + [least] * (count - 1), total - largest - least * (count - 1)
    while rest > 0:
        movable = [i for i in range(1, count) if given[i] < largest] or [i for i in range(1, count) if given[i] < most]
        pool, budget = sum([loads[i] for i in movable]), rest
        for i in movable:
            addition = min(most - given[i], max(1, budget * loads[i] // pool), rest)
            given[i] = given[i] + addition
            rest = rest - addition
    return np.array(given)


def noise(key, dims, deviation, reach, cuts=(), kind=jnp.bfloat16):
    values = deviation * jax.random.normal(key, dims, jnp.float32)
    if cuts:
        values = values * level_of(key, dims, cuts, -0.22, 0.18)
    return jnp.clip(values, -reach, reach).astype(kind)


def setup_inputs(seed: int = 0, part: int = 0) -> dict:
    splits = jax.random.split(jax.random.key(seed), 19)
    part_splits = jax.random.split(jax.random.fold_in(splits[18], part), 19)
    resid_in = noise(part_splits[0], (TOKENS, D), 1.0, 6.0, ((0, 8),))
    norm_attn = jnp.clip(1.0 + 0.18 * jax.random.normal(splits[1], (D,), jnp.float32), 0.1, 1.9)
    norm_moe = jnp.clip(1.0 + 0.18 * jax.random.normal(splits[2], (D,), jnp.float32), 0.1, 1.9)
    w_query = noise(splits[3], (D, HEADS * HEAD), D ** -0.5, 0.125, ((0, 8), (1, 2)))
    w_key = noise(splits[4], (D, KV_HEADS * HEAD), D ** -0.5, 0.125, ((0, 8), (1, 2)))
    w_value = noise(splits[5], (D, KV_HEADS * HEAD), D ** -0.5, 0.125, ((0, 8), (1, 2)))
    head_offset = draw_head_offset(jax.random.fold_in(splits[18], 71), part)
    kv_cache = noise(part_splits[7], (TOKENS, LEN, KV_HEADS, 2 * HEAD), 1.0, 6.0, ((0, 8), (2, 2)))
    lengths = draw_lengths(jax.random.fold_in(jax.random.fold_in(splits[18], part), 71), part)
    w_output = noise(splits[9], (HEADS * HEAD, D), (HEADS * HEAD // 4) ** -0.5, 0.375, ((0, 2), (1, 8)))
    routes_keys = jax.random.split(jax.random.fold_in(part_splits[10], 1), TOKENS // SEQ_DEV)
    routes_turns = jax.random.permutation(jax.random.fold_in(part_splits[10], 3), TOKENS // SEQ_DEV)
    routes = jax.vmap(lambda own, number: routed_block(jax.random.fold_in(part_splits[10], 2), own, number, SEQ_DEV, EXPERTS, TOPK, CAP, 1))(routes_keys, routes_turns).reshape((TOKENS, TOPK))
    route_weights = jnp.clip(0.2 + 0.8 * jax.random.uniform(part_splits[11], (TOKENS, TOPK), jnp.float32) ** level_of(part_splits[11], (TOKENS, TOPK), ((0, 8),), -0.2, 0.2), 0.2, 1.0)
    gate_experts = noise(splits[12], (EXPERTS, D, FE), D ** -0.5, 0.125, ((0, 8), (2, 2)))
    up_experts = noise(splits[13], (EXPERTS, D, FE), D ** -0.5, 0.125, ((0, 8), (2, 2)))
    down_experts = noise(splits[14], (EXPERTS, FE, D), FE ** -0.5, 0.25, ((0, 8), (1, 2)))
    gate_shared = noise(splits[15], (D, FS), D ** -0.5, 0.125, ((0, 8), (1, 2)))
    up_shared = noise(splits[16], (D, FS), D ** -0.5, 0.125, ((0, 8), (1, 2)))
    down_shared = noise(splits[17], (FS, D), FS ** -0.5, 0.25, ((0, 2), (1, 8)))
    return {"resid_in": resid_in, "norm_attn": norm_attn, "norm_moe": norm_moe, "w_query": w_query, "w_key": w_key, "w_value": w_value, "head_offset": head_offset, "kv_cache": kv_cache, "lengths": lengths, "w_output": w_output, "routes": routes, "route_weights": route_weights, "gate_experts": gate_experts, "up_experts": up_experts, "down_experts": down_experts, "gate_shared": gate_shared, "up_shared": up_shared, "down_shared": down_shared}


EPS = 1e-06

def rms_scale(row_block, gain):
    rows_wide = row_block.astype(jnp.float32)
    inverse = lax.rsqrt(lax.optimization_barrier(jnp.mean(rows_wide * rows_wide, axis=-1, keepdims=True)) + EPS)
    return rows_wide * inverse * gain.astype(jnp.float32)

def grouped_sum(left_rows, right_rows, groups):
    group_width = left_rows.shape[1] // groups
    running = jnp.zeros((left_rows.shape[0], right_rows.shape[1]), jnp.float32)
    for group_idx in range(groups):
        low = group_idx * group_width
        partial_prod = jnp.dot(left_rows[:, low:low + group_width], right_rows[low:low + group_width], preferred_element_type=jnp.float32)
        rounded = lax.optimization_barrier(partial_prod.astype(jnp.bfloat16))
        running = running + rounded.astype(jnp.float32)
    return running

def reference(resid_in, norm_attn, norm_moe, w_query, w_key, w_value, head_offset, kv_cache, lengths, w_output, routes, route_weights, gate_experts, up_experts, down_experts, gate_shared, up_shared, down_shared):
    seq_count = resid_in.shape[0]
    normed = rms_scale(resid_in, norm_attn).astype(jnp.bfloat16)
    query = jnp.dot(normed, w_query, preferred_element_type=jnp.float32).astype(jnp.bfloat16)
    key_new = jnp.dot(normed, w_key, preferred_element_type=jnp.float32).astype(jnp.bfloat16)
    value_new = jnp.dot(normed, w_value, preferred_element_type=jnp.float32).astype(jnp.bfloat16)
    new_rows = jnp.concatenate([key_new.reshape(seq_count, KV_HEADS, HEAD), value_new.reshape(seq_count, KV_HEADS, HEAD)], axis=2)
    offsets = head_offset.astype(jnp.float32).reshape(KV_HEADS, HEADS // KV_HEADS, 1)

    def stick_one(inputs):
        query_row, cache_rows, length_one = inputs
        query_heads = query_row.astype(jnp.float32).reshape(KV_HEADS, HEADS // KV_HEADS, HEAD)
        key_rows = cache_rows[:, :, :HEAD].astype(jnp.float32)
        value_rows = cache_rows[:, :, HEAD:].astype(jnp.float32)
        scores = jnp.einsum('kgd,lkd->kgl', query_heads, key_rows) * HEAD ** (-0.5) - offsets
        alive_mask = (jnp.arange(LEN, dtype=jnp.int32) < length_one)[None, None, :]
        remain = jnp.where(alive_mask, jax.nn.log_sigmoid(-scores), 0.0)
        suffix = lax.cumsum(remain, axis=2, reverse=True) - remain
        stick = jnp.where(alive_mask, jnp.exp(jax.nn.log_sigmoid(scores) + suffix), 0.0)
        stick = lax.optimization_barrier(stick.astype(jnp.bfloat16))
        mixed_out = jnp.einsum('kgl,lkd->kgd', stick.astype(jnp.float32), value_rows)
        return mixed_out.reshape(HEADS * HEAD).astype(jnp.bfloat16)
    attended = lax.map(stick_one, (query, kv_cache, lengths))
    attn_sum = grouped_sum(attended, w_output, N_TP)
    resid_mid = (resid_in.astype(jnp.float32) + attn_sum).astype(jnp.bfloat16)
    normed_moe = rms_scale(resid_mid, norm_moe).astype(jnp.bfloat16)
    gate_s = jnp.dot(normed_moe, gate_shared, preferred_element_type=jnp.float32)
    up_s = jnp.dot(normed_moe, up_shared, preferred_element_type=jnp.float32)
    hidden_shared = (jax.nn.silu(gate_s) * up_s).astype(jnp.bfloat16)
    shared_out = grouped_sum(hidden_shared, down_shared, N_TP)
    flat_routes = routes.reshape(-1)
    flat_weights = jnp.concatenate([route_weights.reshape(-1).astype(jnp.float32), jnp.zeros((1,), jnp.float32)])
    padded_rows = jnp.concatenate([normed_moe, jnp.zeros((1, D), jnp.bfloat16)], axis=0)
    most_rows = CAP * N_EP

    def expert_term(expert_id):
        picked = jnp.nonzero(flat_routes == expert_id, size=most_rows, fill_value=flat_routes.shape[0])[0].astype(jnp.int32)
        token_ids = picked // TOPK
        rows_in = padded_rows[token_ids]
        gate_h = jnp.dot(rows_in, gate_experts[expert_id], preferred_element_type=jnp.float32)
        up_h = jnp.dot(rows_in, up_experts[expert_id], preferred_element_type=jnp.float32)
        hidden_e = (jax.nn.silu(gate_h) * up_h).astype(jnp.bfloat16)
        expert_out = lax.optimization_barrier(grouped_sum(hidden_e, down_experts[expert_id], N_TP).astype(jnp.bfloat16))
        return (expert_out.astype(jnp.float32) * flat_weights[picked][:, None], token_ids)
    terms, token_all = lax.map(expert_term, jnp.arange(EXPERTS, dtype=jnp.int32))
    routed = jnp.zeros((seq_count + 1, D), jnp.float32).at[token_all.reshape(-1)].add(terms.reshape(-1, D))
    layer_out = (resid_mid.astype(jnp.float32) + shared_out + routed[:seq_count]).astype(jnp.bfloat16)
    return (layer_out, new_rows)
```

```python
import functools

import jax
import jax.numpy as jnp
from jax import lax
from jax.experimental import pallas as pl
from jax.experimental.pallas import tpu as pltpu
from jax.sharding import PartitionSpec as P

HEAD = 64
CORES = 2
LANES = 128
EPS = 1e-06
F32 = jnp.float32
BF16 = jnp.bfloat16


def inverse_rms(rows_wide):
    return lax.rsqrt(jnp.mean(rows_wide * rows_wide, axis=-1, keepdims=True) + EPS)


def core_swap(x):
    n_ep = lax.axis_size("ep")
    return lax.ppermute(x, "ep", [(i, i ^ 1) for i in range(n_ep)])


def z_send(x, step):
    n_ep = lax.axis_size("ep")
    return lax.ppermute(x, "ep", [(i, (i + CORES * step) % n_ep) for i in range(n_ep)])


def pick(x, index, axis=0):
    return lax.dynamic_index_in_dim(x, index, axis, keepdims=False)


def gather_ep(x):
    n_z = lax.axis_size("ep") // CORES
    me = lax.axis_index("ep")
    z, core = me // CORES, me % CORES
    line = jnp.stack([x] + [z_send(x, -s) for s in range(1, n_z)])
    other = core_swap(line)
    both = jnp.stack([jnp.where(core == 0, line, other), jnp.where(core == 0, other, line)], axis=1)
    ordered = lax.dynamic_slice_in_dim(jnp.concatenate([both, both]), (n_z - z) % n_z, n_z, 0)
    return ordered.reshape((n_z * CORES,) + x.shape)


def spread_ep(x):
    return lax.all_to_all(x, "ep", 0, 0, tiled=True)


def sum_over_tp(x):
    n_tp = lax.axis_size("tp")
    total = x.astype(F32)
    for s in range(1, n_tp):
        total = total + lax.ppermute(x, "tp", [(i, (i + s) % n_tp) for i in range(n_tp)]).astype(F32)
    return total


def scatter_sum(x):
    n_ep, n_tp = lax.axis_size("ep"), lax.axis_size("tp")
    n_z = n_ep // CORES
    me, t = lax.axis_index("ep"), lax.axis_index("tp")
    z, core = me // CORES, me % CORES
    _, rows, cols = x.shape
    grid = x.reshape(n_z, CORES, rows, cols)
    part = pick(grid, core, 1).astype(F32) + core_swap(pick(grid, 1 - core, 1).astype(BF16)).astype(F32)
    width = cols // n_tp
    total = lax.dynamic_slice_in_dim(part, t * width, width, 2)
    for s in range(1, n_tp):
        piece = lax.dynamic_slice_in_dim(part, (t + s) % n_tp * width, width, 2).astype(BF16)
        total = total + lax.ppermute(piece, "tp", [(i, (i + s) % n_tp) for i in range(n_tp)]).astype(F32)
    mine = pick(total, z)
    for s in range(1, n_z):
        mine = mine + z_send(pick(total, (z + s) % n_z).astype(BF16), s).astype(F32)
    return mine


def stick_kernel(lengths, query, offsets, kv_hbm, out, kv, high, low, gain, sems, *, kv_local, per_group):
    seqs, rows, _ = query.shape
    width = kv.shape[1]
    blocks = width // LANES
    copies = [pltpu.make_async_copy(kv_hbm.at[i], kv.at[i], sems.at[i]) for i in range(seqs)]
    for copy in copies:
        copy.start()
    column = lax.broadcasted_iota(jnp.int32, (rows, width), 1)
    head = lax.broadcasted_iota(jnp.int32, (rows, width), 0)
    own = (column % kv_local) == (head // per_group)
    offset = offsets[...]

    def alive(i):
        return own & (column < lengths[i] * kv_local)

    for i in range(seqs):
        copies[i].wait()
        scores = lax.dot_general(
            query[i], kv[i], (((1,), (1,)), ((), ())), preferred_element_type=F32
        )
        scores = scores * HEAD ** (-0.5) - offset
        tail = jnp.log1p(jnp.exp(-jnp.abs(scores)))
        remain = jnp.where(alive(i), jnp.minimum(-scores, 0.0) - tail, 0.0)
        gain[i] = jnp.minimum(scores, 0.0) - tail
        remain = jnp.concatenate([remain[:, b * LANES : (b + 1) * LANES] for b in range(blocks)], axis=0)
        upper = remain.astype(BF16)
        high[i] = upper
        low[i] = (remain - upper.astype(F32)).astype(BF16)
    left = lax.broadcasted_iota(jnp.int32, (LANES, 2 * LANES), 0)
    right = lax.broadcasted_iota(jnp.int32, (LANES, 2 * LANES), 1)
    later = jnp.where((left > right) | (right >= LANES), 1.0, 0.0).astype(BF16)
    for i in range(seqs):
        sums = jnp.dot(high[i], later, preferred_element_type=F32) + jnp.dot(
            low[i], later, preferred_element_type=F32
        )
        carry = jnp.zeros((rows, LANES), F32)
        suffix = [None] * blocks
        for b in range(blocks - 1, -1, -1):
            block = sums[b * rows : (b + 1) * rows]
            suffix[b] = block[:, :LANES] + carry
            carry = carry + block[:, LANES:]
        power = gain[i] + jnp.concatenate(suffix, axis=1)
        stick = jnp.where(alive(i), jnp.exp(power), 0.0).astype(BF16)
        out[i] = jnp.dot(stick, kv[i], preferred_element_type=F32).astype(BF16)


def stick_read(query, kv_cache, lengths, offsets):
    seqs, cache_len, kv_local, pair = kv_cache.shape
    heads = offsets.shape[0]
    rows = -(-heads // 8) * 8
    width = cache_len * kv_local
    padded = jnp.pad(query.reshape(seqs, heads, HEAD), ((0, 0), (0, rows - heads), (0, pair - HEAD)))
    offset_rows = jnp.pad(offsets, (0, rows - heads)).reshape(rows, 1)
    blocks = width // LANES
    mixed = pl.pallas_call(
        functools.partial(stick_kernel, kv_local=kv_local, per_group=heads // kv_local),
        out_shape=jax.ShapeDtypeStruct((seqs, rows, pair), BF16),
        in_specs=[
            pl.BlockSpec(memory_space=pltpu.SMEM),
            pl.BlockSpec(memory_space=pltpu.VMEM),
            pl.BlockSpec(memory_space=pltpu.VMEM),
            pl.BlockSpec(memory_space=pl.ANY),
        ],
        out_specs=pl.BlockSpec(memory_space=pltpu.VMEM),
        scratch_shapes=[
            pltpu.VMEM((seqs, width, pair), BF16),
            pltpu.VMEM((seqs, blocks * rows, LANES), BF16),
            pltpu.VMEM((seqs, blocks * rows, LANES), BF16),
            pltpu.VMEM((seqs, rows, width), F32),
            pltpu.SemaphoreType.DMA((seqs,)),
        ],
        name="stick_read",
    )(lengths, padded, offset_rows, kv_cache.reshape(seqs, width, pair))
    return mixed[:, :heads, HEAD:].reshape(seqs, heads * HEAD)


def on_device(
    resid_in,
    norm_attn,
    norm_moe,
    w_query,
    w_key,
    w_value,
    head_offset,
    kv_cache,
    lengths,
    w_output,
    routes,
    route_weights,
    gate_experts,
    up_experts,
    down_experts,
    gate_shared,
    up_shared,
    down_shared,
):
    toks, width = resid_in.shape
    n_ep, n_tp = lax.axis_size("ep"), lax.axis_size("tp")
    me = lax.axis_index("ep")
    local_experts = gate_experts.shape[0]
    part = width // n_ep
    all_toks = n_ep * toks

    units = gate_shared.shape[1] // n_ep
    gates = jnp.stack([gate_shared, up_shared]).reshape(2, part, n_ep, units).transpose(2, 0, 1, 3)
    downs = down_shared.reshape(n_ep, units * down_shared.shape[1])
    dealt = jnp.concatenate([gates.reshape(n_ep, -1), downs], axis=1)
    split = 2 * part * units
    end = dealt.shape[1]
    dealt = jnp.pad(dealt, ((0, 0), (0, -end % LANES)))
    dealt = spread_ep(dealt.reshape(n_ep, -1, LANES)).reshape(n_ep, -1)
    shared_in = dealt[:, :split].reshape(n_ep, 2, part, units).transpose(1, 0, 2, 3).reshape(2, width, units)
    shared_down = dealt[:, split:end].reshape(n_ep, units, part).transpose(1, 0, 2).reshape(units, width)

    expert_ids = lax.broadcasted_iota(jnp.int32, (1, 1, n_ep * local_experts), 2)
    table = jnp.sum(jnp.where(routes[:, :, None] == expert_ids, route_weights[:, :, None], 0.0), axis=1)
    table_high = lax.reduce_precision(table, 8, 7)
    table_low = lax.reduce_precision(table - table_high, 8, 7)
    tables = jnp.stack([table_high, table_low], axis=1).astype(BF16)
    tables = tables.reshape(toks, 2, n_ep, local_experts).transpose(2, 0, 1, 3).reshape(n_ep, toks, -1)
    tables = jnp.pad(tables, ((0, 0), (0, 0), (0, -tables.shape[2] % LANES)))
    columns = resid_in.reshape(toks, n_ep, part).transpose(1, 0, 2)
    first = spread_ep(jnp.concatenate([columns, tables], axis=2)).reshape(all_toks, -1)
    resid_cols = first[:, :part].astype(F32)
    weights = first[:, part : part + 2 * local_experts].astype(F32)
    weights = weights[:, :local_experts] + weights[:, local_experts:]

    gained = (resid_cols * lax.dynamic_slice_in_dim(norm_attn, me * part, part)).astype(BF16)
    w_all = jnp.concatenate([w_query, w_key, w_value], axis=1)
    partial_qkv = jnp.dot(gained, w_all, preferred_element_type=F32).astype(BF16)
    arrived = spread_ep(partial_qkv.reshape(n_ep, toks, -1))
    resid_wide = resid_in.astype(F32)
    qkv = (jnp.sum(arrived.astype(F32), axis=0) * inverse_rms(resid_wide)).astype(BF16)
    q_cols, k_cols = w_query.shape[1], w_key.shape[1]
    kv_local = k_cols // HEAD
    key_new = qkv[:, q_cols : q_cols + k_cols].reshape(toks, kv_local, HEAD)
    value_new = qkv[:, q_cols + k_cols :].reshape(toks, kv_local, HEAD)
    new_rows = jnp.concatenate([key_new, value_new], axis=2)
    attended = stick_read(qkv[:, :q_cols], kv_cache, lengths, head_offset)

    attended_all = spread_ep(jnp.broadcast_to(attended[None], (n_ep,) + attended.shape))
    attn_part = jnp.dot(
        attended_all.reshape(all_toks, -1), w_output, preferred_element_type=F32
    ).astype(BF16)
    mid_cols = (resid_cols + sum_over_tp(attn_part)).astype(BF16)
    resid_mid = gather_ep(mid_cols).transpose(1, 0, 2).reshape(all_toks, width)
    mid_wide = resid_mid.astype(F32)
    normed_moe = (mid_wide * inverse_rms(mid_wide) * norm_moe).astype(BF16)

    def hidden(gate, up):
        gate_h = jnp.dot(normed_moe, gate, preferred_element_type=F32)
        up_h = jnp.dot(normed_moe, up, preferred_element_type=F32)
        return (jax.nn.silu(gate_h) * up_h).astype(BF16)

    total = jnp.dot(hidden(shared_in[0], shared_in[1]), shared_down, preferred_element_type=F32)
    for e in range(local_experts):
        hidden_e = hidden(gate_experts[e], up_experts[e])
        out_e = jnp.dot(hidden_e, down_experts[e], preferred_element_type=F32)
        total = total + jnp.where(weights[:, e : e + 1] != 0.0, out_e * weights[:, e : e + 1], 0.0)
    moe_out = scatter_sum(total.reshape(n_ep, toks, width))
    own_rows = lax.dynamic_slice(
        resid_mid, (me * toks, lax.axis_index("tp") * (width // n_tp)), (toks, width // n_tp)
    )
    layer_out = (own_rows.astype(F32) + moe_out).astype(BF16)
    return (layer_out, new_rows)


def solution(mesh):
    return jax.shard_map(
        on_device,
        mesh=mesh,
        in_specs=(
            P(("grp", "ep"), None),
            P(),
            P(),
            P("ep", "tp"),
            P("ep", "tp"),
            P("ep", "tp"),
            P("tp"),
            P(("grp", "ep"), None, "tp", None),
            P(("grp", "ep")),
            P("tp", "ep"),
            P(("grp", "ep"), None),
            P(("grp", "ep"), None),
            P("ep", None, "tp"),
            P("ep", None, "tp"),
            P("ep", "tp", None),
            P("ep", "tp"),
            P("ep", "tp"),
            P("tp", "ep"),
        ),
        out_specs=(P(("grp", "ep"), "tp"), P(("grp", "ep"), "tp", None)),
        check_vma=False,
    )
```

```python
import functools

import jax
import jax.numpy as jnp
from jax import lax
from jax.experimental import pallas as pl
from jax.experimental.pallas import tpu as pltpu
from jax.sharding import PartitionSpec as P

HEAD = 64
CORES = 2
LANES = 128
EPS = 1e-06
F32 = jnp.float32
BF16 = jnp.bfloat16


def inverse_rms(rows_wide):
    return lax.rsqrt(jnp.mean(rows_wide * rows_wide, axis=-1, keepdims=True) + EPS)


def core_swap(x):
    n_ep = lax.axis_size("ep")
    return lax.ppermute(x, "ep", [(i, i ^ 1) for i in range(n_ep)])


def z_send(x, step):
    n_ep = lax.axis_size("ep")
    return lax.ppermute(x, "ep", [(i, (i + CORES * step) % n_ep) for i in range(n_ep)])


def pick(x, index, axis=0):
    return lax.dynamic_index_in_dim(x, index, axis, keepdims=False)


def gather_ep(x):
    n_z = lax.axis_size("ep") // CORES
    line = jnp.stack([x] + [z_send(x, -s) for s in range(1, n_z)])
    return line, core_swap(line)


def in_order(line, other):
    n_z = line.shape[0]
    me = lax.axis_index("ep")
    z, core = me // CORES, me % CORES
    both = jnp.stack([jnp.where(core == 0, line, other), jnp.where(core == 0, other, line)], axis=1)
    ordered = lax.dynamic_slice_in_dim(jnp.concatenate([both, both]), (n_z - z) % n_z, n_z, 0)
    return ordered.reshape((n_z * CORES,) + line.shape[1:])


def spread_ep(x):
    return lax.all_to_all(x, "ep", 0, 0, tiled=True)


def sum_over_tp(x):
    n_tp = lax.axis_size("tp")
    total = x.astype(F32)
    for s in range(1, n_tp):
        total = total + lax.ppermute(x, "tp", [(i, (i + s) % n_tp) for i in range(n_tp)]).astype(F32)
    return total


def scatter_sum(x):
    n_ep, n_tp = lax.axis_size("ep"), lax.axis_size("tp")
    n_z = n_ep // CORES
    me, t = lax.axis_index("ep"), lax.axis_index("tp")
    z, core = me // CORES, me % CORES
    _, rows, cols = x.shape
    grid = x.reshape(n_z, CORES, rows, cols)
    part = pick(grid, core, 1).astype(F32) + core_swap(pick(grid, 1 - core, 1).astype(BF16)).astype(F32)
    width = cols // n_tp
    total = lax.dynamic_slice_in_dim(part, t * width, width, 2)
    for s in range(1, n_tp):
        piece = lax.dynamic_slice_in_dim(part, (t + s) % n_tp * width, width, 2).astype(BF16)
        total = total + lax.ppermute(piece, "tp", [(i, (i + s) % n_tp) for i in range(n_tp)]).astype(F32)
    mine = pick(total, z)
    for s in range(1, n_z):
        mine = mine + z_send(pick(total, (z + s) % n_z).astype(BF16), s).astype(F32)
    return mine


def stick_kernel(lengths, query, offsets, kv_hbm, out, kv, high, low, gain, sems, *, kv_local, per_group):
    seqs, rows, _ = query.shape
    width = kv.shape[1]
    blocks = width // LANES
    copies = [pltpu.make_async_copy(kv_hbm.at[i], kv.at[i], sems.at[i]) for i in range(seqs)]
    for copy in copies:
        copy.start()
    column = lax.broadcasted_iota(jnp.int32, (rows, width), 1)
    head = lax.broadcasted_iota(jnp.int32, (rows, width), 0)
    own = (column % kv_local) == (head // per_group)
    offset = offsets[...]

    def alive(i):
        return own & (column < lengths[i] * kv_local)

    for i in range(seqs):
        copies[i].wait()
        scores = lax.dot_general(
            query[i], kv[i], (((1,), (1,)), ((), ())), preferred_element_type=F32
        )
        scores = scores * HEAD ** (-0.5) - offset
        tail = jnp.log1p(jnp.exp(-jnp.abs(scores)))
        remain = jnp.where(alive(i), jnp.minimum(-scores, 0.0) - tail, 0.0)
        gain[i] = jnp.minimum(scores, 0.0) - tail
        remain = jnp.concatenate([remain[:, b * LANES : (b + 1) * LANES] for b in range(blocks)], axis=0)
        upper = remain.astype(BF16)
        high[i] = upper
        low[i] = (remain - upper.astype(F32)).astype(BF16)
    left = lax.broadcasted_iota(jnp.int32, (LANES, 2 * LANES), 0)
    right = lax.broadcasted_iota(jnp.int32, (LANES, 2 * LANES), 1)
    later = jnp.where((left > right) | (right >= LANES), 1.0, 0.0).astype(BF16)
    for i in range(seqs):
        sums = jnp.dot(high[i], later, preferred_element_type=F32) + jnp.dot(
            low[i], later, preferred_element_type=F32
        )
        carry = jnp.zeros((rows, LANES), F32)
        suffix = [None] * blocks
        for b in range(blocks - 1, -1, -1):
            block = sums[b * rows : (b + 1) * rows]
            suffix[b] = block[:, :LANES] + carry
            carry = carry + block[:, LANES:]
        power = gain[i] + jnp.concatenate(suffix, axis=1)
        stick = jnp.where(alive(i), jnp.exp(power), 0.0).astype(BF16)
        out[i] = jnp.dot(stick, kv[i], preferred_element_type=F32).astype(BF16)


def stick_read(query, kv_cache, lengths, offsets):
    seqs, cache_len, kv_local, pair = kv_cache.shape
    heads = offsets.shape[0]
    rows = -(-heads // 8) * 8
    width = cache_len * kv_local
    padded = jnp.pad(query.reshape(seqs, heads, HEAD), ((0, 0), (0, rows - heads), (0, pair - HEAD)))
    offset_rows = jnp.pad(offsets, (0, rows - heads)).reshape(rows, 1)
    blocks = width // LANES
    mixed = pl.pallas_call(
        functools.partial(stick_kernel, kv_local=kv_local, per_group=heads // kv_local),
        out_shape=jax.ShapeDtypeStruct((seqs, rows, pair), BF16),
        in_specs=[
            pl.BlockSpec(memory_space=pltpu.SMEM),
            pl.BlockSpec(memory_space=pltpu.VMEM),
            pl.BlockSpec(memory_space=pltpu.VMEM),
            pl.BlockSpec(memory_space=pl.ANY),
        ],
        out_specs=pl.BlockSpec(memory_space=pltpu.VMEM),
        scratch_shapes=[
            pltpu.VMEM((seqs, width, pair), BF16),
            pltpu.VMEM((seqs, blocks * rows, LANES), BF16),
            pltpu.VMEM((seqs, blocks * rows, LANES), BF16),
            pltpu.VMEM((seqs, rows, width), F32),
            pltpu.SemaphoreType.DMA((seqs,)),
        ],
        name="stick_read",
    )(lengths, padded, offset_rows, kv_cache.reshape(seqs, width, pair))
    return mixed[:, :heads, HEAD:].reshape(seqs, heads * HEAD)


def expert_kernel(
    place, line, other, gain, weights, shared_gate, shared_up, shared_down,
    gate_hbm, up_hbm, down_hbm, out, gate, up, down, sems,
):
    n_z, rows, part = line.shape
    experts = gate.shape[0]
    width = n_z * CORES * part
    copies = [
        pltpu.make_async_copy(gate_hbm, gate, sems.at[0]),
        pltpu.make_async_copy(up_hbm, up, sems.at[1]),
        pltpu.make_async_copy(down_hbm, down, sems.at[2]),
    ]
    for copy in copies:
        copy.start()
    pieces = [(s, r, ref) for s in range(n_z) for r, ref in enumerate((line, other))]
    squares = jnp.zeros((rows, 1), F32)
    for s, _, ref in pieces:
        wide = ref[s].astype(F32)
        squares = squares + jnp.sum(wide * wide, axis=1, keepdims=True)
    inverse = lax.rsqrt(squares / width + EPS)
    normed, spans = [], []
    for s, r, ref in pieces:
        core = place[1] if r == 0 else 1 - place[1]
        column = (place[0] + s) % n_z * CORES + core
        normed.append((ref[s].astype(F32) * inverse * gain[column]).astype(BF16))
        spans.append(pl.ds(pl.multiple_of(column * part, part), part))

    def product(take):
        return sum(jnp.dot(x, take(span), preferred_element_type=F32) for x, span in zip(normed, spans))

    def gated(gate_h, up_h):
        return (gate_h / (1.0 + jnp.exp(-gate_h)) * up_h).astype(BF16)

    hidden = gated(product(lambda span: shared_gate[span, :]), product(lambda span: shared_up[span, :]))
    total = jnp.dot(hidden, shared_down[...], preferred_element_type=F32)
    copies[0].wait()
    copies[1].wait()
    hiddens = [
        gated(product(lambda span: gate[e, span, :]), product(lambda span: up[e, span, :]))
        for e in range(experts)
    ]
    copies[2].wait()
    for e in range(experts):
        weight = weights[:, e : e + 1]
        out_e = jnp.dot(hiddens[e], down[e], preferred_element_type=F32)
        total = total + jnp.where(weight != 0.0, out_e * weight, 0.0)
    out[...] = total.astype(BF16)


def run_experts(line, other, gain, weights, shared, gate, up, down):
    n_z, rows, part = line.shape
    width = n_z * CORES * part
    me = lax.axis_index("ep")
    place = jnp.stack([me // CORES, me % CORES]).astype(jnp.int32)
    vmem = pl.BlockSpec(memory_space=pltpu.VMEM)
    hbm = pl.BlockSpec(memory_space=pl.ANY)
    return pl.pallas_call(
        expert_kernel,
        out_shape=jax.ShapeDtypeStruct((rows, width), BF16),
        in_specs=[pl.BlockSpec(memory_space=pltpu.SMEM)] + [vmem] * 7 + [hbm] * 3,
        out_specs=vmem,
        scratch_shapes=[
            pltpu.VMEM(gate.shape, BF16),
            pltpu.VMEM(up.shape, BF16),
            pltpu.VMEM(down.shape, BF16),
            pltpu.SemaphoreType.DMA((3,)),
        ],
        name="run_experts",
    )(place, line, other, gain.reshape(n_z * CORES, 1, part), weights, *shared, gate, up, down)


def on_device(
    resid_in,
    norm_attn,
    norm_moe,
    w_query,
    w_key,
    w_value,
    head_offset,
    kv_cache,
    lengths,
    w_output,
    routes,
    route_weights,
    gate_experts,
    up_experts,
    down_experts,
    gate_shared,
    up_shared,
    down_shared,
):
    toks, width = resid_in.shape
    n_ep, n_tp = lax.axis_size("ep"), lax.axis_size("tp")
    me = lax.axis_index("ep")
    local_experts = gate_experts.shape[0]
    part = width // n_ep
    all_toks = n_ep * toks

    units = gate_shared.shape[1] // n_ep
    gates = jnp.stack([gate_shared, up_shared]).reshape(2, part, n_ep, units).transpose(2, 0, 1, 3)
    downs = down_shared.reshape(n_ep, units * down_shared.shape[1])
    dealt = jnp.concatenate([gates.reshape(n_ep, -1), downs], axis=1)
    split = 2 * part * units
    end = dealt.shape[1]
    dealt = jnp.pad(dealt, ((0, 0), (0, -end % LANES)))
    dealt = spread_ep(dealt.reshape(n_ep, -1, LANES)).reshape(n_ep, -1)
    shared_in = dealt[:, :split].reshape(n_ep, 2, part, units).transpose(1, 0, 2, 3).reshape(2, width, units)
    shared_down = dealt[:, split:end].reshape(n_ep, units, part).transpose(1, 0, 2).reshape(units, width)

    expert_ids = lax.broadcasted_iota(jnp.int32, (1, 1, n_ep * local_experts), 2)
    table = jnp.sum(jnp.where(routes[:, :, None] == expert_ids, route_weights[:, :, None], 0.0), axis=1)
    table_high = lax.reduce_precision(table, 8, 7)
    table_low = lax.reduce_precision(table - table_high, 8, 7)
    tables = jnp.stack([table_high, table_low], axis=1).astype(BF16)
    tables = tables.reshape(toks, 2, n_ep, local_experts).transpose(2, 0, 1, 3).reshape(n_ep, toks, -1)
    tables = jnp.pad(tables, ((0, 0), (0, 0), (0, -tables.shape[2] % LANES)))
    columns = resid_in.reshape(toks, n_ep, part).transpose(1, 0, 2)
    resid_cols = spread_ep(columns).reshape(all_toks, part).astype(F32)

    gained = (resid_cols * lax.dynamic_slice_in_dim(norm_attn, me * part, part)).astype(BF16)
    w_all = jnp.concatenate([w_query, w_key, w_value], axis=1)
    partial_qkv = jnp.dot(gained, w_all, preferred_element_type=F32).astype(BF16)
    arrived = spread_ep(partial_qkv.reshape(n_ep, toks, -1))
    resid_wide = resid_in.astype(F32)
    qkv = (jnp.sum(arrived.astype(F32), axis=0) * inverse_rms(resid_wide)).astype(BF16)
    q_cols, k_cols = w_query.shape[1], w_key.shape[1]
    kv_local = k_cols // HEAD
    key_new = qkv[:, q_cols : q_cols + k_cols].reshape(toks, kv_local, HEAD)
    value_new = qkv[:, q_cols + k_cols :].reshape(toks, kv_local, HEAD)
    new_rows = jnp.concatenate([key_new, value_new], axis=2)
    attended = stick_read(qkv[:, :q_cols], kv_cache, lengths, head_offset)

    heads_out = attended.shape[1]
    sent = jnp.concatenate([jnp.broadcast_to(attended[None], (n_ep,) + attended.shape), tables], axis=2)
    second = spread_ep(sent).reshape(all_toks, -1)
    weights = second[:, heads_out : heads_out + 2 * local_experts].astype(F32)
    weights = weights[:, :local_experts] + weights[:, local_experts:]
    attn_part = jnp.dot(second[:, :heads_out], w_output, preferred_element_type=F32).astype(BF16)
    mid_cols = (resid_cols + sum_over_tp(attn_part)).astype(BF16)
    line, other = gather_ep(mid_cols)

    shared = (shared_in[0], shared_in[1], shared_down)
    total = run_experts(line, other, norm_moe, weights, shared, gate_experts, up_experts, down_experts)
    moe_out = scatter_sum(total.reshape(n_ep, toks, width))
    own = [lax.dynamic_slice_in_dim(half, me * toks, toks, 1) for half in (line, other)]
    resid_mid = in_order(*own).transpose(1, 0, 2).reshape(toks, width)
    own_rows = lax.dynamic_slice_in_dim(resid_mid, lax.axis_index("tp") * (width // n_tp), width // n_tp, 1)
    layer_out = (own_rows.astype(F32) + moe_out).astype(BF16)
    return (layer_out, new_rows)


def solution(mesh):
    return jax.shard_map(
        on_device,
        mesh=mesh,
        in_specs=(
            P(("grp", "ep"), None),
            P(),
            P(),
            P("ep", "tp"),
            P("ep", "tp"),
            P("ep", "tp"),
            P("tp"),
            P(("grp", "ep"), None, "tp", None),
            P(("grp", "ep")),
            P("tp", "ep"),
            P(("grp", "ep"), None),
            P(("grp", "ep"), None),
            P("ep", None, "tp"),
            P("ep", None, "tp"),
            P("ep", "tp", None),
            P("ep", "tp"),
            P("ep", "tp"),
            P("tp", "ep"),
        ),
        out_specs=(P(("grp", "ep"), "tp"), P(("grp", "ep"), "tp", None)),
        check_vma=False,
    )
```
